32 devices in a mesh: fs: 8 (over z, y), tp: 4 (over x, core).
Axes of the slice: x: 2, y: 2, z: 4, core: 2. Of those that a mesh axis runs over, the one named last changes fastest.
Arguments:
- prompt_tokens: bfloat16 [768, 4096], P('tp'), may hold values from -6 to 6
- norm_gain: float32 [4096], P('fs'), may hold values from 0.1 to 1.9
- gate_trained: float32 [4096, 11264], P('fs', 'tp'), may hold values from -0.09375 to 0.09375
- up_trained: float32 [4096, 11264], P('fs', 'tp'), may hold values from -0.09375 to 0.09375
- down_trained: float32 [11264, 4096], P('fs', 'tp'), may hold values from -0.078125 to 0.078125
Outputs:
- gate_serving: bfloat16 [4096, 11264], P(None, 'fs')
- up_serving: bfloat16 [4096, 11264], P(None, 'fs')
- down_serving: bfloat16 [11264, 4096], P('fs')
- mixed: bfloat16 [768, 4096], P('tp', 'fs')
The draws below stay inside these ranges and needn't reach their ends.
All inputs are finite; a program needn't handle non-finite values.
Results may differ from the reference program's by a relative error of at most 0.0082.
Values may be sent and summed in bfloat16 or wider, within the bound.
A program may use at most 128 MiB of HBM per device.

```python
import jax
import jax.numpy as jnp
from jax import lax

D = 4096
FF = 11264
TOKENS = 768


def with_spikes(entries, key, source, target, shards_of, factor):
    def block_of(dim):
        return (jnp.arange(entries.shape[dim]) // (entries.shape[dim] // shards_of)).reshape((-1,) + (1,) * (entries.ndim - 1 - dim))

    near = jax.random.permutation(key, shards_of)[block_of(target)]
    second = (block_of(target) + shards_of // 2) % shards_of
    return jnp.where((block_of(source) == near) | (block_of(source) == second), factor * entries, entries)


def levels(stream_key, extent, shards, low, high):
    def one(axis_at, blocks):
        heights = jax.random.uniform(jax.random.fold_in(jax.random.fold_in(stream_key, 6), axis_at), (blocks,), jnp.float32, low / len(shards), high / len(shards))
        return jnp.repeat(jnp.exp(heights), extent[axis_at] // blocks).reshape((-1,) + (1,) * (len(extent) - axis_at - 1))

    level = one(*shards[0])
    for cut in shards[1:]:
        level = level * one(*cut)
    return level


def scatter_about(stream_key, dims, scale, reach, cuts=(), dtype=jnp.bfloat16):
    entries = scale * jax.random.normal(stream_key, dims, jnp.float32)
    if cuts:
        entries = entries * levels(stream_key, dims, cuts, -0.22, 0.18)
    return jnp.clip(entries, -reach, reach).astype(dtype)


def heavy_noise(stream_key, dims, scale, bound, shards, heavy, dtype=jnp.bfloat16):
    values = scale * jax.random.normal(stream_key, dims, jnp.float32)
    if shards:
        values = values * levels(stream_key, dims, shards, -0.22, 0.18)
    return jnp.clip(with_spikes(values, jax.random.fold_in(stream_key, 3), *heavy), -bound, bound).astype(dtype)


def setup_inputs(seed: int = 0) -> dict:
    splits = jax.random.split(jax.random.key(seed), 6)
    return {
        "prompt_tokens": scatter_about(splits[0], (TOKENS, D), 1.0, 6.0, ((0, 4),)),
        "norm_gain": jnp.clip(1.0 + 0.18 * jax.random.normal(splits[1], (D,), jnp.float32), 0.1, 1.9),
        "gate_trained": scatter_about(splits[2], (D, FF), D ** -0.5, 0.09375, ((0, 8), (1, 4)), jnp.float32),
        "up_trained": scatter_about(splits[3], (D, FF), D ** -0.5, 0.09375, ((0, 8), (1, 4)), jnp.float32),
        "down_trained": heavy_noise(splits[4], (FF, D), FF ** -0.5, 0.078125, ((0, 8), (1, 4)), (0, 1, 8, 2.0), jnp.float32),
    }


def reference(prompt_tokens, norm_gain, gate_trained, up_trained, down_trained):
    gate_serving = (gate_trained * norm_gain[:, None]).astype(jnp.bfloat16)
    up_serving = (up_trained * norm_gain[:, None]).astype(jnp.bfloat16)
    down_serving = down_trained.astype(jnp.bfloat16)
    tokens = prompt_tokens.astype(jnp.float32)
    scale = jax.lax.rsqrt(lax.optimization_barrier(jnp.mean(tokens * tokens, axis=-1, keepdims=True)) + 1e-06)
    normed = (tokens * scale).astype(jnp.bfloat16)
    gate = jnp.dot(normed, gate_serving, preferred_element_type=jnp.float32)
    up = jnp.dot(normed, up_serving, preferred_element_type=jnp.float32)
    hidden = (jax.nn.silu(gate) * up).astype(jnp.bfloat16)
    mixed = jnp.dot(hidden, down_serving, preferred_element_type=jnp.float32).astype(jnp.bfloat16)
    return (gate_serving, up_serving, down_serving, mixed)
```

```python
import functools

import jax
import jax.numpy as jnp
from jax import lax
from jax.experimental import pallas as pl
from jax.experimental.pallas import tpu as pltpu
from jax.sharding import PartitionSpec as P

MESH = pl.DeviceIdType.MESH
HOME, AWAY, BOTH = 0, 1, 2
LAYER_VMEM = 27 * 2 ** 20


SHARES = ((1, AWAY), (2, BOTH), (4, AWAY), (7, HOME), (6, BOTH), (6, BOTH), (6, BOTH))


def chunk_plan(rows):
    unit = max(16, rows // sum(share for share, _ in SHARES) // 16 * 16)
    plan, at = [], 0
    for i, (share, way) in enumerate(SHARES):
        size = rows - at if i == len(SHARES) - 1 else share * unit
        plan.append((at, size, way))
        at += size
    return tuple(plan)


def layer_kernel(fs, tp, plan, pieces, tok_hbm, gain, gate_f32, up_f32, down_f32,
                 out, dout, mixed, part, w, gcol, stage, dstage, tok, scale, nrm, acc, hidden,
                 pcross, pown, ybuf, sbuf, zbuf,
                 part_send, part_recv, own_send, relay_send, land_recv,
                 sib_send, sib_recv, cross_send, down_send, down_recv,
                 stage_sem, dstage_sem, tok_sem, keep_sem, ysend, yrecv, zsend, zrecv):
    f, t = lax.axis_index("fs"), lax.axis_index("tp")
    x, c = t // 2, lax.rem(t, 2)
    z, y = f // 2, lax.rem(f, 2)
    source_f32 = (gate_f32, up_f32)
    rows, wide = gate_f32.shape
    width = out.shape[2]
    units, dcols = down_f32.shape
    tokens = tok.shape[0]
    features = dout.shape[1]
    block_width = features // fs
    planes = fs // 2
    half = fs // 2
    sib, far = 2 * x + 1 - c, 2 * (1 - x) + c
    chunks = len(plan)
    slots = stage.shape[0]
    casts = [(k, g) for k in range(chunks) for g in range(2)]

    def fetch(i):
        k, g = casts[i]
        at, size, _ = plan[k]
        return pltpu.make_async_copy(
            source_f32[g].at[pl.ds(at, size), :], stage.at[i % slots, pl.ds(0, size), :], stage_sem.at[i % slots])

    depth = units // pieces

    def dfetch(i):
        return pltpu.make_async_copy(
            down_f32.at[pl.ds(i * depth, depth), :], dstage.at[i % 2], dstage_sem.at[i % 2])

    take_tok = pltpu.make_async_copy(tok_hbm, tok, tok_sem)
    for i in range(slots):
        fetch(i).start()
    for i in range(2):
        dfetch(i).start()
    take_tok.start()

    me = f * tp + t
    barrier = pltpu.get_barrier_semaphore()
    for i in range(1, fs * tp):
        other = lax.rem(me + i, fs * tp)
        pl.semaphore_signal(barrier, inc=1, device_id=(other // tp, lax.rem(other, tp)), device_id_type=MESH)
    gcol[...] = jnp.broadcast_to(gain[...], (128, rows)).T
    pl.semaphore_wait(barrier, fs * tp - 1)

    own_cross = z // 2 != x
    part_cross = z // 2 == x
    at_home = z // 2 == x
    true = f >= 0

    def uses(cross, way, dropped):
        return jnp.logical_not(cross) if way == dropped else true

    def remote(src, dst, ssem, rsem, fs_to, tp_to):
        return pltpu.make_async_remote_copy(
            src_ref=src, dst_ref=dst, send_sem=ssem, recv_sem=rsem,
            device_id=(fs_to, tp_to), device_id_type=MESH)

    sent = []

    def send(cond, copy):
        @pl.when(cond)
        def _():
            copy.start()
        sent.append((cond, copy))

    def to_serve(view, sems, k, cond, home, g):
        at, size, _ = plan[k]
        for yy in range(2):
            to = 2 * home + yy
            here = jnp.logical_and(to == f, c == g)
            send(jnp.logical_and(cond, jnp.logical_not(here)), remote(
                view(pl.ds(at, size), pl.ds(yy * width, width)),
                out.at[g, pl.ds(f * rows + at, size), :],
                sems.at[g, yy, k], land_recv.at[f, k], to, 2 * x + g))

    def part_copy(g, k):
        at, size, _ = plan[k]
        return remote(w.at[g, pl.ds(at, size), :], part.at[g, pl.ds(at, size), :],
                      part_send.at[g, k], part_recv.at[g, k], f, far)

    def give(i):
        k, g = casts[i]
        send(uses(own_cross, plan[k][2], HOME), part_copy(g, k))
        to_serve(lambda r, q: w.at[g, r, q], own_send, k, uses(own_cross, plan[k][2], AWAY), t, g)

    for i, (k, g) in enumerate(casts):
        at, size, _ = plan[k]
        fetch(i).wait()

        @pl.loop(0, size // 16)
        def _(r):
            r = pl.multiple_of(r * 16, 16)
            gains = gcol[pl.ds(at + r, 16), :]
            for j in range(wide // 128):
                lanes = pl.ds(j * 128, 128)
                w[g, pl.ds(at + r, 16), lanes] = (stage[i % slots, pl.ds(r, 16), lanes] * gains).astype(w.dtype)
        if i + slots < len(casts):
            fetch(i + slots).start()
        if i:
            give(i - 1)

    block = pl.ds(pl.multiple_of(t * dcols, dcols), dcols)
    for i in range(pieces):
        dfetch(i).wait()

        @pl.loop(0, depth // 16)
        def _(r):
            r = pl.multiple_of(r * 16, 16)
            dout[pl.ds(i * depth + r, 16), block] = dstage[i % 2, pl.ds(r, 16), :].astype(dout.dtype)
        if i + 2 < pieces:
            dfetch(i + 2).start()
        if i == 0:
            give(len(casts) - 1)

    take_tok.wait()
    step = 32

    @pl.loop(0, tokens // step)
    def _(i):
        some = pl.ds(pl.multiple_of(i * step, step), step)
        v = tok[some, :].astype(jnp.float32)
        scale[some, :] = lax.rsqrt(jnp.mean(v * v, axis=-1, keepdims=True) + 1e-06)

    down_far = remote(dout.at[:, block], dout.at[:, block], down_send.at[0], down_recv.at[0], f, far)
    down_sib = remote(dout.at[:, block], dout.at[:, block], down_send.at[1], down_recv.at[1], f, sib)
    send(true, down_far)
    send(true, down_sib)

    @pl.loop(0, fs)
    def _(s):
        v = tok[:, pl.ds(pl.multiple_of(s * rows, rows), rows)].astype(jnp.float32)
        v = (v * scale[...]).astype(nrm.dtype)
        for k, (at, size, _) in enumerate(plan):
            nrm[k, s, :, pl.ds(0, size)] = v[:, at:at + size]
    acc[...] = jnp.zeros_like(acc)

    for k in range(chunks):
        come = uses(part_cross, plan[k][2], HOME)

        @pl.when(come)
        def _():
            for g in range(2):
                part_copy(g, k).wait_recv()
        for g in range(2):
            to_serve(lambda r, q: part.at[g, r, q], relay_send, k, come, lax.rem(t + 2, tp), g)

    keeps = lax.rem(z, 2) == c
    mine = pl.ds(pl.multiple_of(f * rows, rows), rows)
    kept_copy = pltpu.make_async_copy(
        part.at[c, :, pl.ds(pl.multiple_of(y * width, 128), width)], out.at[c, mine, :], keep_sem)

    @pl.when(jnp.logical_and(keeps, jnp.logical_not(at_home)))
    def _():
        kept_copy.start()
        kept_copy.wait()

    @pl.when(jnp.logical_and(keeps, at_home))
    def _():
        @pl.loop(0, rows // 16)
        def _(r):
            r = pl.multiple_of(r * 16, 16)
            to = pl.multiple_of(f * rows + r, 16)
            out[c, pl.ds(to, 16), :] = w[c, pl.ds(r, 16), pl.ds(pl.multiple_of(y * width, 128), width)]

    def landed(g, k, source):
        at, size, _ = plan[k]
        return out.at[g, pl.ds(pl.multiple_of(source * rows + at, 16), size), :]

    def crossing(k, source):
        ref = landed(c, k, source)
        return remote(ref, ref, cross_send.at[source, k], land_recv.at[source, k], f, far)

    def beside(g, k, source):
        ref = landed(g, k, source)
        return remote(ref, ref, sib_send.at[source, k], sib_recv.at[source, k], f, sib)

    def arrive(k, source, cross):
        @pl.when(jnp.logical_not(jnp.logical_and(keeps, f == source)))
        def _():
            crossing(k, source).wait_recv()
        if cross:
            crossing(k, source).start()
        beside(c, k, source).start()

    def accumulate(k, source):
        at, size, _ = plan[k]
        beside(1 - c, k, source).wait_recv()
        left = nrm[k, source, :, pl.ds(0, size)]

        @pl.loop(0, 2)
        def _(g):
            acc[g] += jnp.dot(left, out[g, pl.ds(pl.multiple_of(source * rows + at, 16), size), :],
                              preferred_element_type=jnp.float32)

    same = (f // half) * half
    turned = half - same

    def side(k):
        return at_home if plan[k][2] == HOME else jnp.logical_not(at_home)

    one_way = [k for k in range(chunks) if plan[k][2] != BOTH]
    both_ways = [k for k in range(chunks) if plan[k][2] == BOTH]
    for k in one_way:
        @pl.when(side(k))
        def _():
            @pl.loop(0, half)
            def _(i):
                arrive(k, turned + i, True)
    for k in one_way:
        @pl.loop(0, half)
        def _(i):
            arrive(k, same + i, False)
    due = [(k, same, half) for k in one_way]
    for k in both_ways:
        if k == both_ways[-1]:
            down_far.wait_recv()
            fblock = pl.ds(pl.multiple_of(far * dcols, dcols), dcols)
            send(true, remote(dout.at[:, fblock], dout.at[:, fblock], down_send.at[2], down_recv.at[2], f, sib))

        @pl.loop(0, fs)
        def _(i):
            arrive(k, i, False)
        for kk, base, count in due:
            @pl.loop(0, count)
            def _(i):
                accumulate(kk, base + i)
        due = [(k, 0, fs)]
    for k in one_way:
        @pl.when(jnp.logical_not(side(k)))
        def _():
            @pl.loop(0, half)
            def _(i):
                arrive(k, turned + i, False)
    for kk, base, count in due + [(k, turned, half) for k in one_way]:
        @pl.loop(0, count)
        def _(i):
            accumulate(kk, base + i)

    hidden[...] = (jax.nn.silu(acc[0]) * acc[1]).astype(hidden.dtype)
    down_sib.wait_recv()
    remote(dout.at[:, block], dout.at[:, block], down_send.at[2], down_recv.at[2], f, sib).wait_recv()

    def sums(to):
        at = pl.multiple_of(to * block_width, block_width)
        return jnp.dot(hidden[...], dout[:, pl.ds(at, block_width)], preferred_element_type=jnp.float32)

    order = sorted(range(1, planes), key=lambda o: abs(o - planes // 2)) + [0]
    across = {off: remote(pcross.at[off], ybuf.at[off], ysend.at[off], yrecv.at[off], 2 * z + 1 - y, t) for off in order}
    last = None
    for off in order:
        pcross[off] = sums(2 * lax.rem(z + off, planes) + 1 - y).astype(pcross.dtype)
        if last is not None:
            across[last].start()
        last = off
    for i, off in enumerate(order):
        pown[off] = sums(2 * lax.rem(z + off, planes) + y)
        if i == 0:
            across[last].start()
    along = {}
    total = None
    for off in order:
        to = lax.rem(z + off, planes)
        across[off].wait_recv()
        pair = pown[off] + ybuf[off].astype(jnp.float32)
        if off:
            sbuf[off] = pair.astype(sbuf.dtype)
            along[off] = remote(sbuf.at[off], zbuf.at[off], zsend.at[off], zrecv.at[off], 2 * to + y, t)
            along[off].start()
        else:
            total = pair
    for off in order[:-1]:
        along[off].wait_recv()
        total += zbuf[off].astype(jnp.float32)
    mixed[...] = total.astype(mixed.dtype)

    for off in order:
        across[off].wait_send()
        if off:
            along[off].wait_send()
    for cond, copy in sent:
        @pl.when(cond)
        def _():
            copy.wait_send()
    for k in range(chunks):
        @pl.loop(0, fs)
        def _(i):
            beside(c, k, i).wait_send()
        if plan[k][2] != BOTH:
            @pl.when(side(k))
            def _():
                @pl.loop(0, half)
                def _(i):
                    crossing(k, turned + i).wait_send()


def layer(tok, gain, gate, up, down, fs, tp):
    rows, wide = gate.shape
    width = wide * tp // fs
    units, dcols = down.shape
    features = dcols * tp
    tokens = tok.shape[0]
    block_width = features // fs
    plan = chunk_plan(rows)
    n = len(plan)
    widest = max(size for _, size, _ in plan)
    pieces = 8
    bf16 = jnp.bfloat16
    dma = pltpu.SemaphoreType.DMA
    hbm = pl.BlockSpec(memory_space=pltpu.HBM)
    vmem = pl.BlockSpec(memory_space=pltpu.VMEM)
    slots = pltpu.VMEM((fs // 2, tokens, block_width), bf16)
    return pl.pallas_call(
        functools.partial(layer_kernel, fs, tp, plan, pieces),
        out_shape=(
            pltpu.VMEM((2, rows * fs, width), bf16),
            pltpu.VMEM((units, features), bf16),
            pltpu.VMEM((tokens, block_width), bf16),
            pltpu.HBM((2, rows, wide), bf16),
        ),
        in_specs=[hbm, vmem, hbm, hbm, hbm],
        out_specs=(vmem, vmem, vmem, hbm),
        scratch_shapes=[
            pltpu.VMEM((2, rows, wide), bf16),
            pltpu.VMEM((rows, 128), jnp.float32),
            pltpu.VMEM((3, widest, wide), jnp.float32),
            pltpu.VMEM((2, units // pieces, dcols), jnp.float32),
            pltpu.VMEM(tok.shape, bf16),
            pltpu.VMEM((tokens, 1), jnp.float32),
            pltpu.VMEM((n, fs, tokens, 128), bf16),
            pltpu.VMEM((2, tokens, width), jnp.float32),
            pltpu.VMEM((tokens, width), bf16),
            slots, pltpu.VMEM((fs // 2, tokens, block_width), jnp.float32), slots, slots, slots,
            dma((2, n)), dma((2, n)), dma((2, 2, n)), dma((2, 2, n)), dma((fs, n)),
            dma((fs, n)), dma((fs, n)), dma((fs, n)), dma((3,)), dma((3,)),
            dma((3,)), dma((2,)), dma, dma,
            dma((fs // 2,)), dma((fs // 2,)), dma((fs // 2,)), dma((fs // 2,)),
        ],
        compiler_params=pltpu.CompilerParams(
            collective_id=0, has_side_effects=True, vmem_limit_bytes=LAYER_VMEM),
    )(tok, gain, gate, up, down)


def deliver_kernel(pairs, *refs):
    srcs, dsts, sems = refs[:pairs[-1][0] + 1], refs[pairs[-1][0] + 1:-1], refs[-1]
    copies = []
    for (i, view, cuts), dst in zip(pairs, dsts):
        src = srcs[i] if view is None else srcs[i].at[view]
        depth = dst.shape[0] // cuts
        copies += [(src.at[pl.ds(k * depth, depth)], dst.at[pl.ds(k * depth, depth)]) for k in range(cuts)]
    copies = [pltpu.make_async_copy(src, dst, sems.at[i]) for i, (src, dst) in enumerate(copies)]
    for copy in copies:
        copy.start()
    for copy in copies:
        copy.wait()


def deliver(srcs, pairs):
    def shape(i, view):
        return srcs[i].shape if view is None else srcs[i].shape[1:]

    return pl.pallas_call(
        functools.partial(deliver_kernel, pairs),
        out_shape=tuple(pltpu.HBM(shape(i, view), srcs[i].dtype) for i, view, _ in pairs),
        in_specs=[pl.BlockSpec(memory_space=pltpu.VMEM)] * len(srcs),
        out_specs=(pl.BlockSpec(memory_space=pltpu.HBM),) * len(pairs),
        scratch_shapes=[pltpu.SemaphoreType.DMA((sum(cuts for _, _, cuts in pairs),))],
        compiler_params=pltpu.CompilerParams(vmem_limit_bytes=2 ** 20),
    )(*srcs)


def by_kernels(prompt_tokens, norm_gain, gate_trained, up_trained, down_trained):
    fs, tp = lax.axis_size("fs"), lax.axis_size("tp")
    both, down, mixed, _ = layer(
        prompt_tokens, norm_gain[None, :], gate_trained, up_trained, down_trained, fs, tp)
    gate_serving, up_serving = deliver((both,), ((0, 0, 8), (0, 1, 8)))
    down_serving, mixed = deliver((down, mixed), ((0, None, 8), (1, None, 1)))
    return gate_serving, up_serving, down_serving, mixed


def gather_by_collectives(gate_cast, up_cast, down_cast):
    fs_count = lax.axis_size("fs")
    down_serving = lax.all_gather(down_cast, "tp", axis=1, tiled=True)

    def serve(cast):
        part = lax.all_to_all(cast, "tp", split_axis=0, concat_axis=1, tiled=True)
        mid = lax.all_to_all(part, "fs", split_axis=1, concat_axis=0, tiled=True)
        share, width = mid.shape[0] // fs_count, mid.shape[1]
        blocks = lax.all_gather(mid.reshape(fs_count, share, width), "tp", axis=1, tiled=True)
        return blocks.reshape(-1, width)

    return serve(gate_cast), serve(up_cast), down_serving


def on_device(prompt_tokens, norm_gain, gate_trained, up_trained, down_trained):
    fs, tp = lax.axis_size("fs"), lax.axis_size("tp")
    routed = fs == 2 * tp and tp == 4
    if routed:
        return by_kernels(prompt_tokens, norm_gain, gate_trained, up_trained, down_trained)
    gate_cast = (gate_trained * norm_gain[:, None]).astype(jnp.bfloat16)
    up_cast = (up_trained * norm_gain[:, None]).astype(jnp.bfloat16)
    down_cast = down_trained.astype(jnp.bfloat16)
    gate_serving, up_serving, down_serving = gather_by_collectives(gate_cast, up_cast, down_cast)
    tokens = prompt_tokens.astype(jnp.float32)
    scale = lax.rsqrt(jnp.mean(tokens * tokens, axis=-1, keepdims=True) + 1e-06)
    normed = (tokens * scale).astype(jnp.bfloat16)
    contract = (((0,), (1,)), ((), ()))
    gate_cols = lax.dot_general(gate_serving, normed, contract, preferred_element_type=jnp.float32)
    up_cols = lax.dot_general(up_serving, normed, contract, preferred_element_type=jnp.float32)
    hidden_cols = (jax.nn.silu(gate_cols) * up_cols).astype(jnp.bfloat16)
    summed = lax.psum_scatter(
        lax.dot_general(
            down_serving, hidden_cols, (((0,), (0,)), ((), ())), preferred_element_type=jnp.float32
        ),
        "fs",
        scatter_dimension=0,
        tiled=True,
    )
    mixed = summed.T.astype(jnp.bfloat16)
    return (gate_serving, up_serving, down_serving, mixed)


def solution(mesh):
    return jax.shard_map(
        on_device,
        mesh=mesh,
        in_specs=(P("tp", None), P("fs"), P("fs", "tp"), P("fs", "tp"), P("fs", "tp")),
        out_specs=(P(None, "fs"), P(None, "fs"), P("fs", None), P("tp", "fs")),
        check_vma=False,
    )
```

```python
import functools

import jax
import jax.numpy as jnp
from jax import lax
from jax.experimental import pallas as pl
from jax.experimental.pallas import tpu as pltpu
from jax.sharding import PartitionSpec as P

MESH = pl.DeviceIdType.MESH
HOME, AWAY, BOTH = 0, 1, 2
LAYER_VMEM = 27 * 2 ** 20
EARLY_RELAY = 8


SHARES = ((1, AWAY), (2, BOTH), (4, AWAY), (7, HOME), (2, AWAY), (5, BOTH), (4, BOTH), (4, BOTH), (3, BOTH))
DOWN_CUTS = 8
HALVES = 2


def chunk_plan(rows):
    unit = max(16, rows // sum(share for share, _ in SHARES) // 16 * 16)
    sizes = [share * unit for share, _ in SHARES]
    sizes[-1] += rows - sum(sizes)
    at, plan = 0, [None] * len(SHARES)
    for both in (False, True):
        for i, (_, way) in enumerate(SHARES):
            if (way == BOTH) == both:
                plan[i] = (at, sizes[i], way)
                at += sizes[i]
    return tuple(plan)


def groups_of(plan):
    one_way = [k for k, (_, _, way) in enumerate(plan) if way != BOTH]
    both_ways = [k for k, (_, _, way) in enumerate(plan) if way == BOTH]
    middle = len(both_ways) // 2
    return one_way, both_ways[:middle], both_ways[middle:]


def layer_kernel(fs, tp, plan, pieces, tok_hbm, gain, gate_f32, up_f32, down_f32,
                 out, dout, mixed, part, w, gcol, stage, dstage, tok, scale, nrm, acc, hidden,
                 pcross, pown, ybuf, sbuf, zbuf,
                 part_send, part_recv, own_send, relay_send, land_recv,
                 sib_send, sib_recv, cross_send, down_send, down_recv, sibling_send, sibling_recv,
                 stage_sem, dstage_sem, tok_sem, keep_sem, ysend, yrecv, zsend, zrecv):
    f, t = lax.axis_index("fs"), lax.axis_index("tp")
    x, c = t // 2, lax.rem(t, 2)
    z, y = f // 2, lax.rem(f, 2)
    source_f32 = (gate_f32, up_f32)
    rows, wide = gate_f32.shape
    width = out.shape[2]
    units, dcols = down_f32.shape
    tokens = tok.shape[0]
    features = dout.shape[1]
    block_width = features // fs
    planes = fs // 2
    half = fs // 2
    sib, far = 2 * x + 1 - c, 2 * (1 - x) + c
    chunks = len(plan)
    slots = stage.shape[0]
    groups = groups_of(plan)
    spans = [(plan[group[0]][0], sum(plan[k][1] for k in group)) for group in groups]
    casts = [(k, g) for k in range(chunks) for g in range(2)]

    def fetch(i):
        k, g = casts[i]
        at, size, _ = plan[k]
        return pltpu.make_async_copy(
            source_f32[g].at[pl.ds(at, size), :], stage.at[i % slots, pl.ds(0, size), :], stage_sem.at[i % slots])

    depth = units // pieces

    def dfetch(i):
        return pltpu.make_async_copy(
            down_f32.at[pl.ds(i * depth, depth), :], dstage.at[i % 2], dstage_sem.at[i % 2])

    take_tok = pltpu.make_async_copy(tok_hbm, tok, tok_sem)
    for i in range(slots):
        fetch(i).start()
    for i in range(2):
        dfetch(i).start()
    take_tok.start()

    me = f * tp + t
    barrier = pltpu.get_barrier_semaphore()
    for i in range(1, fs * tp):
        other = lax.rem(me + i, fs * tp)
        pl.semaphore_signal(barrier, inc=1, device_id=(other // tp, lax.rem(other, tp)), device_id_type=MESH)
    gcol[...] = jnp.broadcast_to(gain[...], (128, rows)).T
    pl.semaphore_wait(barrier, fs * tp - 1)

    own_cross = z // 2 != x
    part_cross = z // 2 == x
    at_home = z // 2 == x
    true = f >= 0

    def uses(cross, way, dropped):
        return jnp.logical_not(cross) if way == dropped else true

    def remote(src, dst, ssem, rsem, fs_to, tp_to):
        return pltpu.make_async_remote_copy(
            src_ref=src, dst_ref=dst, send_sem=ssem, recv_sem=rsem,
            device_id=(fs_to, tp_to), device_id_type=MESH)

    sent = []

    def send(cond, copy):
        @pl.when(cond)
        def _():
            copy.start()
        sent.append((cond, copy))

    def to_serve(view, sems, k, cond, home, g):
        at, size, _ = plan[k]
        for yy in range(2):
            to = 2 * home + yy
            here = jnp.logical_and(to == f, c == g)
            send(jnp.logical_and(cond, jnp.logical_not(here)), remote(
                view(pl.ds(at, size), pl.ds(yy * width, width)),
                out.at[g, pl.ds(f * rows + at, size), :],
                sems.at[g, yy, k], land_recv.at[f, k], to, 2 * x + g))

    def part_copy(g, k):
        at, size, _ = plan[k]
        return remote(w.at[g, pl.ds(at, size), :], part.at[g, pl.ds(at, size), :],
                      part_send.at[g, k], part_recv.at[g, k], f, far)

    def give(i):
        k, g = casts[i]
        send(uses(own_cross, plan[k][2], HOME), part_copy(g, k))
        if plan[k][2] != AWAY:
            to_serve(lambda r, q: w.at[g, r, q], own_send, k, own_cross, t, g)

    def relay(k):
        come = uses(part_cross, plan[k][2], HOME)

        @pl.when(come)
        def _():
            for g in range(2):
                part_copy(g, k).wait_recv()
        for g in range(2):
            to_serve(lambda r, q: part.at[g, r, q], relay_send, k, come, lax.rem(t + 2, tp), g)
        for g in range(2):
            to_serve(lambda r, q: w.at[g, r, q], own_send, k, at_home, t, g)

    for i, (k, g) in enumerate(casts):
        at, size, _ = plan[k]
        fetch(i).wait()

        @pl.loop(0, size // 16)
        def _(r):
            r = pl.multiple_of(r * 16, 16)
            gains = gcol[pl.ds(at + r, 16), :]
            for j in range(wide // 128):
                lanes = pl.ds(j * 128, 128)
                w[g, pl.ds(at + r, 16), lanes] = (stage[i % slots, pl.ds(r, 16), lanes] * gains).astype(w.dtype)
        if i + slots < len(casts):
            fetch(i + slots).start()
        if i:
            give(i - 1)
        if i == EARLY_RELAY:
            relay(0)

    block = pl.ds(pl.multiple_of(t * dcols, dcols), dcols)
    for i in range(pieces):
        dfetch(i).wait()

        @pl.loop(0, depth // 16)
        def _(r):
            r = pl.multiple_of(r * 16, 16)
            dout[pl.ds(i * depth + r, 16), block] = dstage[i % 2, pl.ds(r, 16), :].astype(dout.dtype)
        if i + 2 < pieces:
            dfetch(i + 2).start()
        if i == 0:
            give(len(casts) - 1)

    take_tok.wait()
    step = 32

    @pl.loop(0, tokens // step)
    def _(i):
        some = pl.ds(pl.multiple_of(i * step, step), step)
        v = tok[some, :].astype(jnp.float32)
        scale[some, :] = lax.rsqrt(jnp.mean(v * v, axis=-1, keepdims=True) + 1e-06)

    relay(1)
    fblock = pl.ds(pl.multiple_of(far * dcols, dcols), dcols)
    cut = units // DOWN_CUTS

    def down_far(i):
        ref = dout.at[pl.ds(i * cut, cut), block]
        return remote(ref, ref, down_send.at[0, i], down_recv.at[0, i], f, far)

    def down_on(i):
        ref = dout.at[pl.ds(i * cut, cut), fblock]
        return remote(ref, ref, down_send.at[1, i], down_recv.at[1, i], f, sib)

    down_sib = remote(dout.at[:, block], dout.at[:, block], sibling_send, sibling_recv, f, sib)
    for i in range(DOWN_CUTS):
        send(jnp.logical_not(at_home), down_far(i))
    send(true, down_sib)

    @pl.loop(0, fs)
    def _(s):
        v = tok[:, pl.ds(pl.multiple_of(s * rows, rows), rows)].astype(jnp.float32)
        v = (v * scale[...]).astype(nrm.dtype)
        for j, (at, size) in enumerate(spans):
            nrm[j, s, :, pl.ds(0, size)] = v[:, at:at + size]
    acc[...] = jnp.zeros_like(acc)

    for k in range(2, chunks):
        relay(k)

    keeps = lax.rem(z, 2) == c
    mine = pl.ds(pl.multiple_of(f * rows, rows), rows)
    kept_copy = pltpu.make_async_copy(
        part.at[c, :, pl.ds(pl.multiple_of(y * width, 128), width)], out.at[c, mine, :], keep_sem)

    @pl.when(jnp.logical_and(keeps, jnp.logical_not(at_home)))
    def _():
        kept_copy.start()
        kept_copy.wait()

    @pl.when(jnp.logical_and(keeps, at_home))
    def _():
        @pl.loop(0, rows // 16)
        def _(r):
            r = pl.multiple_of(r * 16, 16)
            to = pl.multiple_of(f * rows + r, 16)
            out[c, pl.ds(to, 16), :] = w[c, pl.ds(r, 16), pl.ds(pl.multiple_of(y * width, 128), width)]

    def landed(g, k, source):
        at, size, _ = plan[k]
        return out.at[g, pl.ds(pl.multiple_of(source * rows + at, 16), size), :]

    def crossing(k, source):
        ref = landed(c, k, source)
        return remote(ref, ref, cross_send.at[source, k], land_recv.at[source, k], f, far)

    def beside(g, k, source):
        ref = landed(g, k, source)
        return remote(ref, ref, sib_send.at[source, k], sib_recv.at[source, k], f, sib)

    def arrive(k, source, cross):
        @pl.when(jnp.logical_not(jnp.logical_and(keeps, f == source)))
        def _():
            crossing(k, source).wait_recv()
        if cross:
            crossing(k, source).start()
        beside(c, k, source).start()

    def accumulate(j, source):
        at, size = spans[j]
        for k in groups[j]:
            beside(1 - c, k, source).wait_recv()
        left = nrm[j, source, :, pl.ds(0, size)]

        @pl.loop(0, 2)
        def _(g):
            acc[g] += jnp.dot(left, out[g, pl.ds(pl.multiple_of(source * rows + at, 16), size), :],
                              preferred_element_type=jnp.float32)

    same = (f // half) * half
    turned = half - same

    def side(k):
        return at_home if plan[k][2] == HOME else jnp.logical_not(at_home)

    def pass_on(cond, cuts):
        for i in cuts:
            @pl.when(cond)
            def _():
                down_far(i).wait_recv()
            send(cond, down_on(i))

    one_way, early, late = groups
    for k in one_way:
        @pl.when(side(k))
        def _():
            @pl.loop(0, half)
            def _(i):
                arrive(k, turned + i, True)
    for i in range(DOWN_CUTS):
        send(at_home, down_far(i))
    for k in one_way:
        @pl.loop(0, half)
        def _(i):
            arrive(k, same + i, False)
    for k in early:
        @pl.loop(0, fs)
        def _(i):
            arrive(k, i, False)

    @pl.loop(0, half)
    def _(i):
        accumulate(0, same + i)
    for k in late[:-1]:
        @pl.loop(0, fs)
        def _(i):
            arrive(k, i, False)
        if k == late[0]:
            @pl.loop(0, fs)
            def _(i):
                accumulate(1, i)
    pass_on(at_home, range(DOWN_CUTS))
    pass_on(jnp.logical_not(at_home), range(DOWN_CUTS // 2))
    for k in one_way:
        @pl.when(jnp.logical_not(side(k)))
        def _():
            @pl.loop(0, half)
            def _(i):
                arrive(k, turned + i, False)

    @pl.loop(0, half)
    def _(i):
        arrive(late[-1], same + i, False)
        accumulate(0, turned + i)

    @pl.loop(0, half)
    def _(i):
        arrive(late[-1], turned + i, False)
        accumulate(2, same + i)

    @pl.loop(0, half)
    def _(i):
        accumulate(2, turned + i)

    hidden[...] = (jax.nn.silu(acc[0]) * acc[1]).astype(hidden.dtype)
    down_sib.wait_recv()

    def sums(to):
        at = pl.multiple_of(to * block_width, block_width)
        return jnp.dot(hidden[...], dout[:, pl.ds(at, block_width)], preferred_element_type=jnp.float32)

    order = (3, 2, 1, 0)
    level = {3: 3 - z, 2: lax.rem(z + 2, 4), 1: z + 1 - 2 * lax.rem(z, 2), 0: z}
    def collect(cond):
        @pl.when(cond)
        def _():
            for i in range(DOWN_CUTS):
                down_on(i).wait_recv()

    share = tokens // HALVES
    halves = [pl.ds(h * share, share) for h in range(HALVES)]

    def across(m, h):
        return remote(pcross.at[m, halves[h]], ybuf.at[m, halves[h]], ysend.at[m, h], yrecv.at[m, h], 2 * z + 1 - y, t)

    def along(m, h):
        return remote(sbuf.at[m, halves[h]], zbuf.at[m, halves[h]], zsend.at[m, h], zrecv.at[m, h], 2 * level[m] + y, t)

    def theirs(m):
        pcross[m] = sums(2 * level[m] + 1 - y).astype(pcross.dtype)

    def ours(m):
        pown[m] = sums(2 * level[m] + y)

    def offer(m):
        for h in range(HALVES):
            across(m, h).start()

    def pair(m):
        for h, some in enumerate(halves):
            across(m, h).wait_recv()
            total = pown[m, some] + ybuf[m, some].astype(jnp.float32)
            if m:
                sbuf[m, some] = total.astype(sbuf.dtype)
                along(m, h).start()
            else:
                pown[m, some] = total

    collect(at_home)
    theirs(3)
    theirs(2)
    offer(3)
    ours(3)
    offer(2)
    ours(2)
    pair(3)
    pass_on(jnp.logical_not(at_home), range(DOWN_CUTS // 2, DOWN_CUTS))
    collect(jnp.logical_not(at_home))
    theirs(1)
    theirs(0)
    offer(1)
    ours(1)
    offer(0)
    ours(0)
    for m in (2, 1, 0):
        pair(m)
    total = pown[0]
    for m in (1, 3, 2):
        for h in range(HALVES):
            along(m, h).wait_recv()
        total += zbuf[m].astype(jnp.float32)
    mixed[...] = total.astype(mixed.dtype)

    for m in order:
        for h in range(HALVES):
            across(m, h).wait_send()
            if m:
                along(m, h).wait_send()
    for cond, copy in sent:
        @pl.when(cond)
        def _():
            copy.wait_send()
    for k in range(chunks):
        @pl.loop(0, fs)
        def _(i):
            beside(c, k, i).wait_send()
        if plan[k][2] != BOTH:
            @pl.when(side(k))
            def _():
                @pl.loop(0, half)
                def _(i):
                    crossing(k, turned + i).wait_send()


def layer(tok, gain, gate, up, down, fs, tp):
    rows, wide = gate.shape
    width = wide * tp // fs
    units, dcols = down.shape
    features = dcols * tp
    tokens = tok.shape[0]
    block_width = features // fs
    plan = chunk_plan(rows)
    n = len(plan)
    widest = max(size for _, size, _ in plan)
    pieces = 8
    deepest = max(-(-sum(plan[k][1] for k in group) // 128) * 128 for group in groups_of(plan))
    bf16 = jnp.bfloat16
    dma = pltpu.SemaphoreType.DMA
    hbm = pl.BlockSpec(memory_space=pltpu.HBM)
    vmem = pl.BlockSpec(memory_space=pltpu.VMEM)
    slots = pltpu.VMEM((fs // 2, tokens, block_width), bf16)
    return pl.pallas_call(
        functools.partial(layer_kernel, fs, tp, plan, pieces),
        out_shape=(
            pltpu.VMEM((2, rows * fs, width), bf16),
            pltpu.VMEM((units, features), bf16),
            pltpu.VMEM((tokens, block_width), bf16),
            pltpu.HBM((2, rows, wide), bf16),
        ),
        in_specs=[hbm, vmem, hbm, hbm, hbm],
        out_specs=(vmem, vmem, vmem, hbm),
        scratch_shapes=[
            pltpu.VMEM((2, rows, wide), bf16),
            pltpu.VMEM((rows, 128), jnp.float32),
            pltpu.VMEM((3, widest, wide), jnp.float32),
            pltpu.VMEM((2, units // pieces, dcols), jnp.float32),
            pltpu.VMEM(tok.shape, bf16),
            pltpu.VMEM((tokens, 1), jnp.float32),
            pltpu.VMEM((3, fs, tokens, deepest), bf16),
            pltpu.VMEM((2, tokens, width), jnp.float32),
            pltpu.VMEM((tokens, width), bf16),
            slots, pltpu.VMEM((fs // 2, tokens, block_width), jnp.float32), slots, slots, slots,
            dma((2, n)), dma((2, n)), dma((2, 2, n)), dma((2, 2, n)), dma((fs, n)),
            dma((fs, n)), dma((fs, n)), dma((fs, n)), dma((2, DOWN_CUTS)), dma((2, DOWN_CUTS)), dma, dma,
            dma((3,)), dma((2,)), dma, dma,
            dma((fs // 2, HALVES)), dma((fs // 2, HALVES)), dma((fs // 2, HALVES)), dma((fs // 2, HALVES)),
        ],
        compiler_params=pltpu.CompilerParams(
            collective_id=0, has_side_effects=True, vmem_limit_bytes=LAYER_VMEM),
    )(tok, gain, gate, up, down)


def deliver_kernel(pairs, *refs):
    srcs, dsts, sems = refs[:pairs[-1][0] + 1], refs[pairs[-1][0] + 1:-1], refs[-1]
    copies = []
    for (i, view, cuts), dst in zip(pairs, dsts):
        src = srcs[i] if view is None else srcs[i].at[view]
        depth = dst.shape[0] // cuts
        copies += [(src.at[pl.ds(k * depth, depth)], dst.at[pl.ds(k * depth, depth)]) for k in range(cuts)]
    copies = [pltpu.make_async_copy(src, dst, sems.at[i]) for i, (src, dst) in enumerate(copies)]
    for copy in copies:
        copy.start()
    for copy in copies:
        copy.wait()


def deliver(srcs, pairs):
    def shape(i, view):
        return srcs[i].shape if view is None else srcs[i].shape[1:]

    return pl.pallas_call(
        functools.partial(deliver_kernel, pairs),
        out_shape=tuple(pltpu.HBM(shape(i, view), srcs[i].dtype) for i, view, _ in pairs),
        in_specs=[pl.BlockSpec(memory_space=pltpu.VMEM)] * len(srcs),
        out_specs=(pl.BlockSpec(memory_space=pltpu.HBM),) * len(pairs),
        scratch_shapes=[pltpu.SemaphoreType.DMA((sum(cuts for _, _, cuts in pairs),))],
        compiler_params=pltpu.CompilerParams(vmem_limit_bytes=2 ** 20),
    )(*srcs)


def by_kernels(prompt_tokens, norm_gain, gate_trained, up_trained, down_trained):
    fs, tp = lax.axis_size("fs"), lax.axis_size("tp")
    both, down, mixed, _ = layer(
        prompt_tokens, norm_gain[None, :], gate_trained, up_trained, down_trained, fs, tp)
    gate_serving, up_serving = deliver((both,), ((0, 0, 8), (0, 1, 8)))
    down_serving, mixed = deliver((down, mixed), ((0, None, 8), (1, None, 1)))
    return gate_serving, up_serving, down_serving, mixed


def gather_by_collectives(gate_cast, up_cast, down_cast):
    fs_count = lax.axis_size("fs")
    down_serving = lax.all_gather(down_cast, "tp", axis=1, tiled=True)

    def serve(cast):
        part = lax.all_to_all(cast, "tp", split_axis=0, concat_axis=1, tiled=True)
        mid = lax.all_to_all(part, "fs", split_axis=1, concat_axis=0, tiled=True)
        share, width = mid.shape[0] // fs_count, mid.shape[1]
        blocks = lax.all_gather(mid.reshape(fs_count, share, width), "tp", axis=1, tiled=True)
        return blocks.reshape(-1, width)

    return serve(gate_cast), serve(up_cast), down_serving


def on_device(prompt_tokens, norm_gain, gate_trained, up_trained, down_trained):
    fs, tp = lax.axis_size("fs"), lax.axis_size("tp")
    routed = fs == 2 * tp and tp == 4
    if routed:
        return by_kernels(prompt_tokens, norm_gain, gate_trained, up_trained, down_trained)
    gate_cast = (gate_trained * norm_gain[:, None]).astype(jnp.bfloat16)
    up_cast = (up_trained * norm_gain[:, None]).astype(jnp.bfloat16)
    down_cast = down_trained.astype(jnp.bfloat16)
    gate_serving, up_serving, down_serving = gather_by_collectives(gate_cast, up_cast, down_cast)
    tokens = prompt_tokens.astype(jnp.float32)
    scale = lax.rsqrt(jnp.mean(tokens * tokens, axis=-1, keepdims=True) + 1e-06)
    normed = (tokens * scale).astype(jnp.bfloat16)
    contract = (((0,), (1,)), ((), ()))
    gate_cols = lax.dot_general(gate_serving, normed, contract, preferred_element_type=jnp.float32)
    up_cols = lax.dot_general(up_serving, normed, contract, preferred_element_type=jnp.float32)
    hidden_cols = (jax.nn.silu(gate_cols) * up_cols).astype(jnp.bfloat16)
    summed = lax.psum_scatter(
        lax.dot_general(
            down_serving, hidden_cols, (((0,), (0,)), ((), ())), preferred_element_type=jnp.float32
        ),
        "fs",
        scatter_dimension=0,
        tiled=True,
    )
    mixed = summed.T.astype(jnp.bfloat16)
    return (gate_serving, up_serving, down_serving, mixed)


def solution(mesh):
    return jax.shard_map(
        on_device,
        mesh=mesh,
        in_specs=(P("tp", None), P("fs"), P("fs", "tp"), P("fs", "tp"), P("fs", "tp")),
        out_specs=(P(None, "fs"), P(None, "fs"), P("fs", None), P("tp", "fs")),
        check_vma=False,
    )
```

```python
import functools

import jax
import jax.numpy as jnp
from jax import lax
from jax.experimental import pallas as pl
from jax.experimental.pallas import tpu as pltpu
from jax.sharding import PartitionSpec as P

MESH = pl.DeviceIdType.MESH
HOME, AWAY, BOTH = 0, 1, 2
LAYER_VMEM = 27 * 2 ** 20
EARLY_RELAY = 8
EARLY_CASTS = 2


SHARES = ((1, AWAY), (2, BOTH), (4, AWAY), (7, HOME), (2, AWAY), (6, BOTH), (6, BOTH), (4, BOTH))
DOWN_CUTS = 8
HALVES = 2


def chunk_plan(rows):
    unit = max(16, rows // sum(share for share, _ in SHARES) // 16 * 16)
    sizes = [share * unit for share, _ in SHARES]
    sizes[-1] += rows - sum(sizes)
    at, plan = 0, [None] * len(SHARES)
    for both in (False, True):
        for i, (_, way) in enumerate(SHARES):
            if (way == BOTH) == both:
                plan[i] = (at, sizes[i], way)
                at += sizes[i]
    return tuple(plan)


def groups_of(plan):
    one_way = [k for k, (_, _, way) in enumerate(plan) if way != BOTH]
    both_ways = [k for k, (_, _, way) in enumerate(plan) if way == BOTH]
    middle = len(both_ways) // 2
    return one_way, both_ways[:middle], both_ways[middle:]


def layer_kernel(fs, tp, plan, pieces, tok_hbm, gain, gate_f32, up_f32, down_f32,
                 out, dout, mixed, part, w, gcol, stage, dstage, tok, scale, nrm, acc, hidden,
                 pcross, pown, ybuf, sbuf, zbuf,
                 part_send, part_recv, own_send, relay_send, land_recv,
                 sib_send, sib_recv, cross_send, down_send, down_recv, sibling_send, sibling_recv,
                 stage_sem, dstage_sem, tok_sem, keep_sem, ysend, yrecv, zsend, zrecv):
    f, t = lax.axis_index("fs"), lax.axis_index("tp")
    x, c = t // 2, lax.rem(t, 2)
    z, y = f // 2, lax.rem(f, 2)
    source_f32 = (gate_f32, up_f32)
    rows, wide = gate_f32.shape
    width = out.shape[2]
    units, dcols = down_f32.shape
    tokens = tok.shape[0]
    features = dout.shape[1]
    block_width = features // fs
    planes = fs // 2
    half = fs // 2
    sib, far = 2 * x + 1 - c, 2 * (1 - x) + c
    chunks = len(plan)
    slots = stage.shape[0]
    groups = groups_of(plan)
    spans = [(plan[group[0]][0], sum(plan[k][1] for k in group)) for group in groups]
    casts = [(k, g) for k in range(chunks) for g in range(2)]

    def fetch(i):
        k, g = casts[i]
        at, size, _ = plan[k]
        return pltpu.make_async_copy(
            source_f32[g].at[pl.ds(at, size), :], stage.at[i % slots, pl.ds(0, size), :], stage_sem.at[i % slots])

    depth = units // pieces

    def dfetch(i):
        return pltpu.make_async_copy(
            down_f32.at[pl.ds(i * depth, depth), :], dstage.at[i % 2], dstage_sem.at[i % 2])

    take_tok = pltpu.make_async_copy(tok_hbm, tok, tok_sem)
    for i in range(slots):
        fetch(i).start()
    for i in range(2):
        dfetch(i).start()
    take_tok.start()

    me = f * tp + t
    barrier = pltpu.get_barrier_semaphore()
    for i in range(1, fs * tp):
        other = lax.rem(me + i, fs * tp)
        pl.semaphore_signal(barrier, inc=1, device_id=(other // tp, lax.rem(other, tp)), device_id_type=MESH)
    gcol[...] = jnp.broadcast_to(gain[...], (128, rows)).T

    own_cross = z // 2 != x
    part_cross = z // 2 == x
    at_home = z // 2 == x
    true = f >= 0

    def uses(cross, way, dropped):
        return jnp.logical_not(cross) if way == dropped else true

    def remote(src, dst, ssem, rsem, fs_to, tp_to):
        return pltpu.make_async_remote_copy(
            src_ref=src, dst_ref=dst, send_sem=ssem, recv_sem=rsem,
            device_id=(fs_to, tp_to), device_id_type=MESH)

    sent = []

    def send(cond, copy):
        @pl.when(cond)
        def _():
            copy.start()
        sent.append((cond, copy))

    def to_serve(view, sems, k, cond, home, g):
        at, size, _ = plan[k]
        for yy in range(2):
            to = 2 * home + yy
            here = jnp.logical_and(to == f, c == g)
            send(jnp.logical_and(cond, jnp.logical_not(here)), remote(
                view(pl.ds(at, size), pl.ds(yy * width, width)),
                out.at[g, pl.ds(f * rows + at, size), :],
                sems.at[g, yy, k], land_recv.at[f, k], to, 2 * x + g))

    def part_copy(g, k):
        at, size, _ = plan[k]
        return remote(w.at[g, pl.ds(at, size), :], part.at[g, pl.ds(at, size), :],
                      part_send.at[g, k], part_recv.at[g, k], f, far)

    def cast(i):
        k, g = casts[i]
        at, size, _ = plan[k]
        fetch(i).wait()

        @pl.loop(0, size // 16)
        def _(r):
            r = pl.multiple_of(r * 16, 16)
            gains = gcol[pl.ds(at + r, 16), :]
            for j in range(wide // 128):
                lanes = pl.ds(j * 128, 128)
                w[g, pl.ds(at + r, 16), lanes] = (stage[i % slots, pl.ds(r, 16), lanes] * gains).astype(w.dtype)
        if i + slots < len(casts):
            fetch(i + slots).start()

    def give(i):
        k, g = casts[i]
        send(uses(own_cross, plan[k][2], HOME), part_copy(g, k))
        if plan[k][2] != AWAY:
            to_serve(lambda r, q: w.at[g, r, q], own_send, k, own_cross, t, g)

    def relay(k):
        come = uses(part_cross, plan[k][2], HOME)

        @pl.when(come)
        def _():
            for g in range(2):
                part_copy(g, k).wait_recv()
        for g in range(2):
            to_serve(lambda r, q: part.at[g, r, q], relay_send, k, come, lax.rem(t + 2, tp), g)
        for g in range(2):
            to_serve(lambda r, q: w.at[g, r, q], own_send, k, at_home, t, g)

    for i in range(EARLY_CASTS):
        cast(i)
    pl.semaphore_wait(barrier, fs * tp - 1)
    for i in range(EARLY_CASTS - 1):
        give(i)
    for i in range(EARLY_CASTS, len(casts)):
        cast(i)
        give(i - 1)
        if i == EARLY_RELAY:
            relay(0)

    block = pl.ds(pl.multiple_of(t * dcols, dcols), dcols)
    for i in range(pieces):
        dfetch(i).wait()

        @pl.loop(0, depth // 16)
        def _(r):
            r = pl.multiple_of(r * 16, 16)
            dout[pl.ds(i * depth + r, 16), block] = dstage[i % 2, pl.ds(r, 16), :].astype(dout.dtype)
        if i + 2 < pieces:
            dfetch(i + 2).start()
        if i == 0:
            give(len(casts) - 1)

    take_tok.wait()
    step = 32

    @pl.loop(0, tokens // step)
    def _(i):
        some = pl.ds(pl.multiple_of(i * step, step), step)
        v = tok[some, :].astype(jnp.float32)
        scale[some, :] = lax.rsqrt(jnp.mean(v * v, axis=-1, keepdims=True) + 1e-06)

    relay(1)
    cut = features // fs * 2 // DOWN_CUTS

    def down_cut(home, i):
        at = home * dcols + i % 2 * block_width + i // 2 * cut
        return dout.at[:, pl.ds(pl.multiple_of(at, 128), cut)]

    def down_far(i):
        ref = down_cut(t, i)
        return remote(ref, ref, down_send.at[0, i], down_recv.at[0, i], f, far)

    def down_on(i):
        ref = down_cut(far, i)
        return remote(ref, ref, down_send.at[1, i], down_recv.at[1, i], f, sib)

    down_sib = remote(dout.at[:, block], dout.at[:, block], sibling_send, sibling_recv, f, sib)
    for i in range(DOWN_CUTS):
        send(jnp.logical_not(at_home), down_far(i))
    send(true, down_sib)

    @pl.loop(0, fs)
    def _(s):
        v = tok[:, pl.ds(pl.multiple_of(s * rows, rows), rows)].astype(jnp.float32)
        v = (v * scale[...]).astype(nrm.dtype)
        for j, (at, size) in enumerate(spans):
            nrm[j, s, :, pl.ds(0, size)] = v[:, at:at + size]
    acc[...] = jnp.zeros_like(acc)

    for k in range(2, chunks):
        relay(k)

    keeps = lax.rem(z, 2) == c
    mine = pl.ds(pl.multiple_of(f * rows, rows), rows)
    kept_copy = pltpu.make_async_copy(
        part.at[c, :, pl.ds(pl.multiple_of(y * width, 128), width)], out.at[c, mine, :], keep_sem)

    @pl.when(jnp.logical_and(keeps, jnp.logical_not(at_home)))
    def _():
        kept_copy.start()
        kept_copy.wait()

    @pl.when(jnp.logical_and(keeps, at_home))
    def _():
        @pl.loop(0, rows // 16)
        def _(r):
            r = pl.multiple_of(r * 16, 16)
            to = pl.multiple_of(f * rows + r, 16)
            out[c, pl.ds(to, 16), :] = w[c, pl.ds(r, 16), pl.ds(pl.multiple_of(y * width, 128), width)]

    def landed(g, k, source):
        at, size, _ = plan[k]
        return out.at[g, pl.ds(pl.multiple_of(source * rows + at, 16), size), :]

    def crossing(k, source):
        ref = landed(c, k, source)
        return remote(ref, ref, cross_send.at[source, k], land_recv.at[source, k], f, far)

    def beside(g, k, source):
        ref = landed(g, k, source)
        return remote(ref, ref, sib_send.at[source, k], sib_recv.at[source, k], f, sib)

    def arrive(k, source, cross):
        @pl.when(jnp.logical_not(jnp.logical_and(keeps, f == source)))
        def _():
            crossing(k, source).wait_recv()
        if cross:
            crossing(k, source).start()
        beside(c, k, source).start()

    def accumulate(j, source, gs=(0, 1)):
        at, size = spans[j]
        left = nrm[j, source, :, pl.ds(0, size)]
        for g in gs:
            @pl.when(c != g)
            def _():
                for k in groups[j]:
                    beside(g, k, source).wait_recv()
            acc[g] += jnp.dot(left, out[g, pl.ds(pl.multiple_of(source * rows + at, 16), size), :],
                              preferred_element_type=jnp.float32)

    same = (f // half) * half
    turned = half - same

    def side(k):
        return at_home if plan[k][2] == HOME else jnp.logical_not(at_home)

    def pass_on(cond, cuts):
        for i in cuts:
            @pl.when(cond)
            def _():
                down_far(i).wait_recv()
            send(cond, down_on(i))

    one_way, early, late = groups
    for k in one_way:
        @pl.when(side(k))
        def _():
            @pl.loop(0, half)
            def _(i):
                arrive(k, turned + i, True)
    for i in range(DOWN_CUTS):
        send(at_home, down_far(i))
    for k in one_way:
        @pl.loop(0, half)
        def _(i):
            arrive(k, same + i, False)
    for k in early:
        @pl.loop(0, fs)
        def _(i):
            arrive(k, i, False)

    @pl.loop(0, half)
    def _(i):
        accumulate(0, same + i)
    for k in late[:-1]:
        @pl.loop(0, fs)
        def _(i):
            arrive(k, i, False)
        if k == late[0]:
            @pl.loop(0, fs)
            def _(i):
                accumulate(1, i)
    pass_on(at_home, range(DOWN_CUTS))
    away = jnp.logical_not(at_home)
    pass_on(away, (0, 1))
    for k in one_way:
        @pl.when(jnp.logical_not(side(k)))
        def _():
            @pl.loop(0, half)
            def _(i):
                arrive(k, turned + i, False)

    @pl.loop(0, half)
    def _(i):
        arrive(late[-1], same + i, False)
        accumulate(0, turned + i)

    @pl.loop(0, half)
    def _(i):
        accumulate(2, same + i)
    for g in range(2):
        @pl.when(c == g)
        def _():
            @pl.loop(0, half)
            def _(i):
                arrive(late[-1], turned + i, False)

        @pl.loop(0, half)
        def _(i):
            accumulate(2, turned + i, (g,))

    hidden[...] = (jax.nn.silu(acc[0]) * acc[1]).astype(hidden.dtype)
    down_sib.wait_recv()

    share = block_width // HALVES
    halves = [pl.ds(h * share, share) for h in range(HALVES)]

    def sums(to, h):
        at = pl.multiple_of(to * block_width + h * share, share)
        return jnp.dot(hidden[...], dout[:, pl.ds(at, share)], preferred_element_type=jnp.float32)

    order = (3, 2, 1, 0)
    level = {3: 3 - z, 2: lax.rem(z + 2, 4), 1: z + 1 - 2 * lax.rem(z, 2), 0: z}

    def collect(cond, cuts):
        @pl.when(cond)
        def _():
            for i in cuts:
                down_on(i).wait_recv()

    def across(m, h):
        return remote(pcross.at[m, :, halves[h]], ybuf.at[m, :, halves[h]], ysend.at[m, h], yrecv.at[m, h],
                      2 * z + 1 - y, t)

    def along(m, h):
        return remote(sbuf.at[m, :, halves[h]], zbuf.at[m, :, halves[h]], zsend.at[m, h], zrecv.at[m, h],
                      2 * level[m] + y, t)

    def theirs(m, h):
        pcross[m, :, halves[h]] = sums(2 * level[m] + 1 - y, h).astype(pcross.dtype)

    def ours(m, h):
        pown[m, :, halves[h]] = sums(2 * level[m] + y, h)

    def pair(m, h):
        some = halves[h]
        across(m, h).wait_recv()
        total = pown[m, :, some] + ybuf[m, :, some].astype(jnp.float32)
        if m:
            sbuf[m, :, some] = total.astype(sbuf.dtype)
            along(m, h).start()
        else:
            pown[m, :, some] = total

    collect(at_home, range(DOWN_CUTS))
    first = [(3, 0), (3, 1), (2, 0), (2, 1), (1, 0), (0, 0)]
    second = [(1, 1), (0, 1)]
    for i, step in enumerate(first[:4]):
        theirs(*step)
        if i:
            across(*first[i - 1]).start()
    ours(*first[0])
    across(*first[3]).start()
    pass_on(away, range(2, DOWN_CUTS // 2))
    for step in first[1:4]:
        ours(*step)
    collect(away, range(DOWN_CUTS // 2))
    pair(*first[0])
    pass_on(away, (DOWN_CUTS // 2,))
    theirs(*first[4])
    theirs(*first[5])
    across(*first[4]).start()
    ours(*first[4])
    across(*first[5]).start()
    ours(*first[5])
    pair(*first[1])
    pass_on(away, (DOWN_CUTS // 2 + 1,))
    pair(*first[2])
    pass_on(away, (DOWN_CUTS // 2 + 2,))
    pair(*first[3])
    pass_on(away, range(DOWN_CUTS // 2 + 3, DOWN_CUTS))
    collect(away, range(DOWN_CUTS // 2, DOWN_CUTS))
    for step in second:
        theirs(*step)
    across(*second[0]).start()
    ours(*second[0])
    across(*second[1]).start()
    ours(*second[1])
    for step in first[4:] + second:
        pair(*step)
    total = pown[0]
    for m in (3, 2, 1):
        for h in range(HALVES):
            along(m, h).wait_recv()
        total += zbuf[m].astype(jnp.float32)
    mixed[...] = total.astype(mixed.dtype)

    for m in order:
        for h in range(HALVES):
            across(m, h).wait_send()
            if m:
                along(m, h).wait_send()
    for cond, copy in sent:
        @pl.when(cond)
        def _():
            copy.wait_send()
    for k in range(chunks):
        @pl.loop(0, fs)
        def _(i):
            beside(c, k, i).wait_send()
        if plan[k][2] != BOTH:
            @pl.when(side(k))
            def _():
                @pl.loop(0, half)
                def _(i):
                    crossing(k, turned + i).wait_send()


def layer(tok, gain, gate, up, down, fs, tp):
    rows, wide = gate.shape
    width = wide * tp // fs
    units, dcols = down.shape
    features = dcols * tp
    tokens = tok.shape[0]
    block_width = features // fs
    plan = chunk_plan(rows)
    n = len(plan)
    widest = max(size for _, size, _ in plan)
    pieces = 8
    deepest = max(-(-sum(plan[k][1] for k in group) // 128) * 128 for group in groups_of(plan))
    bf16 = jnp.bfloat16
    dma = pltpu.SemaphoreType.DMA
    hbm = pl.BlockSpec(memory_space=pltpu.HBM)
    vmem = pl.BlockSpec(memory_space=pltpu.VMEM)
    slots = pltpu.VMEM((fs // 2, tokens, block_width), bf16)
    return pl.pallas_call(
        functools.partial(layer_kernel, fs, tp, plan, pieces),
        out_shape=(
            pltpu.VMEM((2, rows * fs, width), bf16),
            pltpu.VMEM((units, features), bf16),
            pltpu.VMEM((tokens, block_width), bf16),
            pltpu.HBM((2, rows, wide), bf16),
        ),
        in_specs=[hbm, vmem, hbm, hbm, hbm],
        out_specs=(vmem, vmem, vmem, hbm),
        scratch_shapes=[
            pltpu.VMEM((2, rows, wide), bf16),
            pltpu.VMEM((rows, 128), jnp.float32),
            pltpu.VMEM((3, widest, wide), jnp.float32),
            pltpu.VMEM((2, units // pieces, dcols), jnp.float32),
            pltpu.VMEM(tok.shape, bf16),
            pltpu.VMEM((tokens, 1), jnp.float32),
            pltpu.VMEM((3, fs, tokens, deepest), bf16),
            pltpu.VMEM((2, tokens, width), jnp.float32),
            pltpu.VMEM((tokens, width), bf16),
            slots, pltpu.VMEM((fs // 2, tokens, block_width), jnp.float32), slots, slots, slots,
            dma((2, n)), dma((2, n)), dma((2, 2, n)), dma((2, 2, n)), dma((fs, n)),
            dma((fs, n)), dma((fs, n)), dma((fs, n)), dma((2, DOWN_CUTS)), dma((2, DOWN_CUTS)), dma, dma,
            dma((3,)), dma((2,)), dma, dma,
            dma((fs // 2, HALVES)), dma((fs // 2, HALVES)), dma((fs // 2, HALVES)), dma((fs // 2, HALVES)),
        ],
        compiler_params=pltpu.CompilerParams(
            collective_id=0, has_side_effects=True, vmem_limit_bytes=LAYER_VMEM),
    )(tok, gain, gate, up, down)


def deliver_kernel(pairs, *refs):
    srcs, dsts, sems = refs[:pairs[-1][0] + 1], refs[pairs[-1][0] + 1:-1], refs[-1]
    copies = []
    for (i, view, cuts), dst in zip(pairs, dsts):
        src = srcs[i] if view is None else srcs[i].at[view]
        depth = dst.shape[0] // cuts
        copies += [(src.at[pl.ds(k * depth, depth)], dst.at[pl.ds(k * depth, depth)]) for k in range(cuts)]
    copies = [pltpu.make_async_copy(src, dst, sems.at[i]) for i, (src, dst) in enumerate(copies)]
    for copy in copies:
        copy.start()
    for copy in copies:
        copy.wait()


def deliver(srcs, pairs):
    def shape(i, view):
        return srcs[i].shape if view is None else srcs[i].shape[1:]

    return pl.pallas_call(
        functools.partial(deliver_kernel, pairs),
        out_shape=tuple(pltpu.HBM(shape(i, view), srcs[i].dtype) for i, view, _ in pairs),
        in_specs=[pl.BlockSpec(memory_space=pltpu.VMEM)] * len(srcs),
        out_specs=(pl.BlockSpec(memory_space=pltpu.HBM),) * len(pairs),
        scratch_shapes=[pltpu.SemaphoreType.DMA((sum(cuts for _, _, cuts in pairs),))],
        compiler_params=pltpu.CompilerParams(vmem_limit_bytes=2 ** 20),
    )(*srcs)


def by_kernels(prompt_tokens, norm_gain, gate_trained, up_trained, down_trained):
    fs, tp = lax.axis_size("fs"), lax.axis_size("tp")
    both, down, mixed, _ = layer(
        prompt_tokens, norm_gain[None, :], gate_trained, up_trained, down_trained, fs, tp)
    gate_serving, up_serving = deliver((both,), ((0, 0, 8), (0, 1, 8)))
    down_serving, mixed = deliver((down, mixed), ((0, None, 8), (1, None, 1)))
    return gate_serving, up_serving, down_serving, mixed


def gather_by_collectives(gate_cast, up_cast, down_cast):
    fs_count = lax.axis_size("fs")
    down_serving = lax.all_gather(down_cast, "tp", axis=1, tiled=True)

    def serve(cast):
        part = lax.all_to_all(cast, "tp", split_axis=0, concat_axis=1, tiled=True)
        mid = lax.all_to_all(part, "fs", split_axis=1, concat_axis=0, tiled=True)
        share, width = mid.shape[0] // fs_count, mid.shape[1]
        blocks = lax.all_gather(mid.reshape(fs_count, share, width), "tp", axis=1, tiled=True)
        return blocks.reshape(-1, width)

    return serve(gate_cast), serve(up_cast), down_serving


def on_device(prompt_tokens, norm_gain, gate_trained, up_trained, down_trained):
    fs, tp = lax.axis_size("fs"), lax.axis_size("tp")
    routed = fs == 2 * tp and tp == 4
    if routed:
        return by_kernels(prompt_tokens, norm_gain, gate_trained, up_trained, down_trained)
    gate_cast = (gate_trained * norm_gain[:, None]).astype(jnp.bfloat16)
    up_cast = (up_trained * norm_gain[:, None]).astype(jnp.bfloat16)
    down_cast = down_trained.astype(jnp.bfloat16)
    gate_serving, up_serving, down_serving = gather_by_collectives(gate_cast, up_cast, down_cast)
    tokens = prompt_tokens.astype(jnp.float32)
    scale = lax.rsqrt(jnp.mean(tokens * tokens, axis=-1, keepdims=True) + 1e-06)
    normed = (tokens * scale).astype(jnp.bfloat16)
    contract = (((0,), (1,)), ((), ()))
    gate_cols = lax.dot_general(gate_serving, normed, contract, preferred_element_type=jnp.float32)
    up_cols = lax.dot_general(up_serving, normed, contract, preferred_element_type=jnp.float32)
    hidden_cols = (jax.nn.silu(gate_cols) * up_cols).astype(jnp.bfloat16)
    summed = lax.psum_scatter(
        lax.dot_general(
            down_serving, hidden_cols, (((0,), (0,)), ((), ())), preferred_element_type=jnp.float32
        ),
        "fs",
        scatter_dimension=0,
        tiled=True,
    )
    mixed = summed.T.astype(jnp.bfloat16)
    return (gate_serving, up_serving, down_serving, mixed)


def solution(mesh):
    return jax.shard_map(
        on_device,
        mesh=mesh,
        in_specs=(P("tp", None), P("fs"), P("fs", "tp"), P("fs", "tp"), P("fs", "tp")),
        out_specs=(P(None, "fs"), P(None, "fs"), P("fs", None), P("tp", "fs")),
        check_vma=False,
    )
```

```python
import functools

import jax
import jax.numpy as jnp
from jax import lax
from jax.experimental import pallas as pl
from jax.experimental.pallas import tpu as pltpu
from jax.sharding import PartitionSpec as P

MESH = pl.DeviceIdType.MESH
HOME, AWAY, BOTH = 0, 1, 2
LAYER_VMEM = 29 * 2 ** 20
EARLY_RELAY = 8
EARLY_CASTS = 2


WAYS = (AWAY, BOTH, AWAY, HOME, AWAY, BOTH, BOTH, BOTH)
SHARES = ((1, 2, 4, 7, 2, 6, 6, 4), (1, 2, 4, 8, 2, 5, 6, 4))
DOWN_CUTS = 8
HALVES = 2


def chunk_plan(rows, shares):
    unit = max(16, rows // sum(shares) // 16 * 16)
    sizes = [share * unit for share in shares]
    sizes[-1] += rows - sum(sizes)
    at, plan = 0, [None] * len(shares)
    for both in (False, True):
        for i, way in enumerate(WAYS):
            if (way == BOTH) == both:
                plan[i] = (at, sizes[i])
                at += sizes[i]
    return tuple(plan)


def groups():
    one_way = [k for k, way in enumerate(WAYS) if way != BOTH]
    both_ways = [k for k, way in enumerate(WAYS) if way == BOTH]
    middle = len(both_ways) // 2
    return one_way, both_ways[:middle], both_ways[middle:]


def spans_of(plans):
    def span(plan, group):
        return plan[group[0]][0], sum(plan[k][1] for k in group)

    spans = [[span(plan, group) for plan in plans] for group in groups()]
    return spans, sorted({pair for both in spans for pair in both})


def layer_kernel(fs, tp, plans, pieces, tok_hbm, gain, gate_f32, up_f32, down_f32,
                 out, dout, mixed, part, w, gcol, stage, dstage, tok, scale, nrm, acc, hidden,
                 pcross, pown, ybuf, sbuf, zbuf,
                 part_send, part_recv, own_send, relay_send, land_recv,
                 sib_send, sib_recv, cross_send, down_send, down_recv, sibling_send, sibling_recv,
                 stage_sem, dstage_sem, tok_sem, keep_sem, ysend, yrecv, zsend, zrecv):
    f, t = lax.axis_index("fs"), lax.axis_index("tp")
    x, c = t // 2, lax.rem(t, 2)
    z, y = f // 2, lax.rem(f, 2)
    source_f32 = (gate_f32, up_f32)
    rows, wide = gate_f32.shape
    width = out.shape[2]
    units, dcols = down_f32.shape
    tokens = tok.shape[0]
    features = dout.shape[1]
    block_width = features // fs
    planes = fs // 2
    half = fs // 2
    sib, far = 2 * x + 1 - c, 2 * (1 - x) + c
    chunks = len(WAYS)
    slots = stage.shape[0]
    one_way, early, late = groups()
    spans, lefts = spans_of(plans)
    casts = [(k, g) for k in range(chunks) for g in range(2)]

    def fetch(i):
        k, g = casts[i]
        at, size = plans[g][k]
        return pltpu.make_async_copy(
            source_f32[g].at[pl.ds(at, size), :], stage.at[i % slots, pl.ds(0, size), :], stage_sem.at[i % slots])

    depth = units // pieces

    def dfetch(i):
        return pltpu.make_async_copy(
            down_f32.at[pl.ds(i * depth, depth), :], dstage.at[i % 2], dstage_sem.at[i % 2])

    take_tok = pltpu.make_async_copy(tok_hbm, tok, tok_sem)
    for i in range(slots):
        fetch(i).start()
    for i in range(2):
        dfetch(i).start()
    take_tok.start()

    me = f * tp + t
    barrier = pltpu.get_barrier_semaphore()
    for i in range(1, fs * tp):
        other = lax.rem(me + i, fs * tp)
        pl.semaphore_signal(barrier, inc=1, device_id=(other // tp, lax.rem(other, tp)), device_id_type=MESH)
    gcol[...] = jnp.broadcast_to(gain[...], (128, rows)).T

    own_cross = z // 2 != x
    part_cross = z // 2 == x
    at_home = z // 2 == x
    true = f >= 0

    def uses(cross, way, dropped):
        return jnp.logical_not(cross) if way == dropped else true

    def remote(src, dst, ssem, rsem, fs_to, tp_to):
        return pltpu.make_async_remote_copy(
            src_ref=src, dst_ref=dst, send_sem=ssem, recv_sem=rsem,
            device_id=(fs_to, tp_to), device_id_type=MESH)

    sent = []

    def send(cond, copy):
        @pl.when(cond)
        def _():
            copy.start()
        sent.append((cond, copy))

    def to_serve(view, sems, k, cond, home, g):
        at, size = plans[g][k]
        for yy in range(2):
            to = 2 * home + yy
            here = jnp.logical_and(to == f, c == g)
            send(jnp.logical_and(cond, jnp.logical_not(here)), remote(
                view(pl.ds(at, size), pl.ds(yy * width, width)),
                out.at[g, pl.ds(f * rows + at, size), :],
                sems.at[g, yy, k], land_recv.at[f, k], to, 2 * x + g))

    def part_copy(g, k):
        at, size = plans[g][k]
        return remote(w.at[g, pl.ds(at, size), :], part.at[g, pl.ds(at, size), :],
                      part_send.at[g, k], part_recv.at[g, k], f, far)

    def cast(i):
        k, g = casts[i]
        at, size = plans[g][k]
        fetch(i).wait()

        @pl.loop(0, size // 16)
        def _(r):
            r = pl.multiple_of(r * 16, 16)
            gains = gcol[pl.ds(at + r, 16), :]
            for j in range(wide // 128):
                lanes = pl.ds(j * 128, 128)
                w[g, pl.ds(at + r, 16), lanes] = (stage[i % slots, pl.ds(r, 16), lanes] * gains).astype(w.dtype)
        if i + slots < len(casts):
            fetch(i + slots).start()

    def give(i):
        k, g = casts[i]
        send(uses(own_cross, WAYS[k], HOME), part_copy(g, k))
        if WAYS[k] != AWAY:
            to_serve(lambda r, q: w.at[g, r, q], own_send, k, own_cross, t, g)

    def relay(k):
        come = uses(part_cross, WAYS[k], HOME)

        @pl.when(come)
        def _():
            for g in range(2):
                part_copy(g, k).wait_recv()
        for g in range(2):
            to_serve(lambda r, q: part.at[g, r, q], relay_send, k, come, lax.rem(t + 2, tp), g)
        for g in range(2):
            to_serve(lambda r, q: w.at[g, r, q], own_send, k, at_home, t, g)

    for i in range(EARLY_CASTS):
        cast(i)
    pl.semaphore_wait(barrier, fs * tp - 1)
    for i in range(EARLY_CASTS - 1):
        give(i)
    for i in range(EARLY_CASTS, len(casts)):
        cast(i)
        give(i - 1)
        if i == EARLY_RELAY:
            relay(0)

    block = pl.ds(pl.multiple_of(t * dcols, dcols), dcols)
    for i in range(pieces):
        dfetch(i).wait()

        @pl.loop(0, depth // 16)
        def _(r):
            r = pl.multiple_of(r * 16, 16)
            dout[pl.ds(i * depth + r, 16), block] = dstage[i % 2, pl.ds(r, 16), :].astype(dout.dtype)
        if i + 2 < pieces:
            dfetch(i + 2).start()
        if i == 0:
            give(len(casts) - 1)

    take_tok.wait()
    step = 32

    @pl.loop(0, tokens // step)
    def _(i):
        some = pl.ds(pl.multiple_of(i * step, step), step)
        v = tok[some, :].astype(jnp.float32)
        scale[some, :] = lax.rsqrt(jnp.mean(v * v, axis=-1, keepdims=True) + 1e-06)

    relay(1)
    cut = features // fs * 2 // DOWN_CUTS

    def down_cut(home, i):
        kind, at = divmod(i, DOWN_CUTS // 2)
        at = home * dcols + (y if kind else 1 - y) * block_width + at * cut
        return dout.at[:, pl.ds(pl.multiple_of(at, 128), cut)]

    def down_far(i):
        ref = down_cut(t, i)
        return remote(ref, ref, down_send.at[0, i], down_recv.at[0, i], f, far)

    def down_on(i):
        ref = down_cut(far, i)
        return remote(ref, ref, down_send.at[1, i], down_recv.at[1, i], f, sib)

    down_sib = remote(dout.at[:, block], dout.at[:, block], sibling_send, sibling_recv, f, sib)
    for i in range(DOWN_CUTS):
        send(jnp.logical_not(at_home), down_far(i))
    send(true, down_sib)

    @pl.loop(0, fs)
    def _(s):
        v = tok[:, pl.ds(pl.multiple_of(s * rows, rows), rows)].astype(jnp.float32)
        v = (v * scale[...]).astype(nrm.dtype)
        for j, (at, size) in enumerate(lefts):
            nrm[j, s, :, pl.ds(0, size)] = v[:, at:at + size]
    acc[...] = jnp.zeros_like(acc)

    for k in range(2, chunks):
        relay(k)

    keeps = lax.rem(z, 2) == c
    mine = pl.ds(pl.multiple_of(f * rows, rows), rows)
    kept_copy = pltpu.make_async_copy(
        part.at[c, :, pl.ds(pl.multiple_of(y * width, 128), width)], out.at[c, mine, :], keep_sem)

    @pl.when(jnp.logical_and(keeps, jnp.logical_not(at_home)))
    def _():
        kept_copy.start()
        kept_copy.wait()

    @pl.when(jnp.logical_and(keeps, at_home))
    def _():
        @pl.loop(0, rows // 16)
        def _(r):
            r = pl.multiple_of(r * 16, 16)
            to = pl.multiple_of(f * rows + r, 16)
            out[c, pl.ds(to, 16), :] = w[c, pl.ds(r, 16), pl.ds(pl.multiple_of(y * width, 128), width)]

    def landed(g, k, source):
        at, size = plans[g][k]
        return out.at[g, pl.ds(pl.multiple_of(source * rows + at, 16), size), :]

    def crossing(g, k, source):
        ref = landed(g, k, source)
        return remote(ref, ref, cross_send.at[source, k], land_recv.at[source, k], f, far)

    def beside(g, k, source):
        ref = landed(g, k, source)
        return remote(ref, ref, sib_send.at[source, k], sib_recv.at[source, k], f, sib)

    def arrive(k, source, cross):
        for g in range(2):
            @pl.when(jnp.logical_and(c == g, jnp.logical_not(jnp.logical_and(keeps, f == source))))
            def _():
                crossing(g, k, source).wait_recv()

            @pl.when(c == g)
            def _():
                if cross:
                    crossing(g, k, source).start()
                beside(g, k, source).start()

    def accumulate(j, source, gs=(0, 1)):
        for g in gs:
            @pl.when(c != g)
            def _():
                for k in groups()[j]:
                    beside(g, k, source).wait_recv()
            at, size = spans[j][g]
            left = nrm[lefts.index((at, size)), source, :, pl.ds(0, size)]
            acc[g] += jnp.dot(left, out[g, pl.ds(pl.multiple_of(source * rows + at, 16), size), :],
                              preferred_element_type=jnp.float32)

    same = (f // half) * half
    turned = half - same

    def side(k):
        return at_home if WAYS[k] == HOME else jnp.logical_not(at_home)

    def pass_on(cond, cuts):
        for i in cuts:
            @pl.when(cond)
            def _():
                down_far(i).wait_recv()
            send(cond, down_on(i))

    for k in one_way:
        @pl.when(side(k))
        def _():
            @pl.loop(0, half)
            def _(i):
                arrive(k, turned + i, True)
    for i in range(DOWN_CUTS):
        send(at_home, down_far(i))
    for k in one_way:
        @pl.loop(0, half)
        def _(i):
            arrive(k, same + i, False)
    for k in early:
        @pl.loop(0, fs)
        def _(i):
            arrive(k, i, False)

    @pl.loop(0, half)
    def _(i):
        accumulate(0, same + i)
    for k in late[:-1]:
        @pl.loop(0, fs)
        def _(i):
            arrive(k, i, False)
        if k == late[0]:
            @pl.loop(0, fs)
            def _(i):
                accumulate(1, i)
    pass_on(at_home, range(DOWN_CUTS))
    away = jnp.logical_not(at_home)
    pass_on(away, (0, 1))
    for k in one_way:
        @pl.when(jnp.logical_not(side(k)))
        def _():
            @pl.loop(0, half)
            def _(i):
                arrive(k, turned + i, False)

    @pl.loop(0, half)
    def _(i):
        arrive(late[-1], same + i, False)
        accumulate(0, turned + i)

    @pl.loop(0, half)
    def _(i):
        accumulate(2, same + i)
    for g in range(2):
        @pl.when(c == g)
        def _():
            @pl.loop(0, half)
            def _(i):
                arrive(late[-1], turned + i, False)

        @pl.loop(0, half)
        def _(i):
            accumulate(2, turned + i, (g,))

    hidden[...] = (jax.nn.silu(acc[0]) * acc[1]).astype(hidden.dtype)
    down_sib.wait_recv()

    share = block_width // HALVES
    halves = [pl.ds(h * share, share) for h in range(HALVES)]

    def sums(to, h):
        at = pl.multiple_of(to * block_width + h * share, share)
        return jnp.dot(hidden[...], dout[:, pl.ds(at, share)], preferred_element_type=jnp.float32)

    order = (3, 2, 1, 0)
    level = {3: 3 - z, 2: lax.rem(z + 2, 4), 1: z + 1 - 2 * lax.rem(z, 2), 0: z}

    def collect(cond, cuts):
        @pl.when(cond)
        def _():
            for i in cuts:
                down_on(i).wait_recv()

    def across(m, h):
        return remote(pcross.at[m, :, halves[h]], ybuf.at[m, :, halves[h]], ysend.at[m, h], yrecv.at[m, h],
                      2 * z + 1 - y, t)

    def along(m, h):
        return remote(sbuf.at[m, :, halves[h]], zbuf.at[m, :, halves[h]], zsend.at[m, h], zrecv.at[m, h],
                      2 * level[m] + y, t)

    def theirs(m, h):
        pcross[m, :, halves[h]] = sums(2 * level[m] + 1 - y, h).astype(pcross.dtype)

    def ours(m, h):
        pown[m, :, halves[h]] = sums(2 * level[m] + y, h)

    def pair(m, h):
        some = halves[h]
        across(m, h).wait_recv()
        total = pown[m, :, some] + ybuf[m, :, some].astype(jnp.float32)
        if m:
            sbuf[m, :, some] = total.astype(sbuf.dtype)
            along(m, h).start()
        else:
            pown[m, :, some] = total

    quarter = DOWN_CUTS // 4
    collect(at_home, range(DOWN_CUTS))
    first = [(3, 0), (3, 1), (2, 0), (2, 1)]
    second = [(1, 0), (1, 1), (0, 0), (0, 1)]
    for i, step in enumerate(first):
        theirs(*step)
        if i:
            across(*first[i - 1]).start()
    ours(*first[0])
    across(*first[3]).start()
    pass_on(away, range(quarter, 2 * quarter))
    ours(*first[1])
    collect(away, range(2 * quarter))
    for i, step in enumerate(second):
        theirs(*step)
        if i:
            across(*second[i - 1]).start()
    ours(*first[2])
    across(*second[3]).start()
    ours(*first[3])
    pair(3, 0)
    pair(3, 1)
    pass_on(away, range(2 * quarter, 3 * quarter))
    pair(2, 0)
    collect(away, range(2 * quarter, 3 * quarter))
    ours(1, 0)
    ours(0, 0)
    pair(2, 1)
    pass_on(away, range(3 * quarter, 4 * quarter - 1))
    pair(1, 0)
    pass_on(away, range(4 * quarter - 1, 4 * quarter))
    collect(away, range(3 * quarter, 4 * quarter))
    ours(1, 1)
    pair(1, 1)
    ours(0, 1)
    pair(0, 0)
    pair(0, 1)
    total = pown[0]
    for m in (3, 2, 1):
        for h in range(HALVES):
            along(m, h).wait_recv()
        total += zbuf[m].astype(jnp.float32)
    mixed[...] = total.astype(mixed.dtype)

    for m in order:
        for h in range(HALVES):
            across(m, h).wait_send()
            if m:
                along(m, h).wait_send()
    for cond, copy in sent:
        @pl.when(cond)
        def _():
            copy.wait_send()
    for g in range(2):
        @pl.when(c == g)
        def _():
            for k in range(chunks):
                @pl.loop(0, fs)
                def _(i):
                    beside(g, k, i).wait_send()
                if WAYS[k] != BOTH:
                    @pl.when(side(k))
                    def _():
                        @pl.loop(0, half)
                        def _(i):
                            crossing(g, k, turned + i).wait_send()


def layer(tok, gain, gate, up, down, fs, tp):
    rows, wide = gate.shape
    width = wide * tp // fs
    units, dcols = down.shape
    features = dcols * tp
    tokens = tok.shape[0]
    block_width = features // fs
    plans = tuple(chunk_plan(rows, shares) for shares in SHARES)
    n = len(WAYS)
    widest = max(size for plan in plans for _, size in plan)
    lefts = spans_of(plans)[1]
    pieces = 8
    deepest = max(-(-size // 128) * 128 for _, size in lefts)
    bf16 = jnp.bfloat16
    dma = pltpu.SemaphoreType.DMA
    hbm = pl.BlockSpec(memory_space=pltpu.HBM)
    vmem = pl.BlockSpec(memory_space=pltpu.VMEM)
    slots = pltpu.VMEM((fs // 2, tokens, block_width), bf16)
    return pl.pallas_call(
        functools.partial(layer_kernel, fs, tp, plans, pieces),
        out_shape=(
            pltpu.VMEM((2, rows * fs, width), bf16),
            pltpu.VMEM((units, features), bf16),
            pltpu.VMEM((tokens, block_width), bf16),
            pltpu.HBM((2, rows, wide), bf16),
        ),
        in_specs=[hbm, vmem, hbm, hbm, hbm],
        out_specs=(vmem, vmem, vmem, hbm),
        scratch_shapes=[
            pltpu.VMEM((2, rows, wide), bf16),
            pltpu.VMEM((rows, 128), jnp.float32),
            pltpu.VMEM((3, widest, wide), jnp.float32),
            pltpu.VMEM((2, units // pieces, dcols), jnp.float32),
            pltpu.VMEM(tok.shape, bf16),
            pltpu.VMEM((tokens, 1), jnp.float32),
            pltpu.VMEM((len(lefts), fs, tokens, deepest), bf16),
            pltpu.VMEM((2, tokens, width), jnp.float32),
            pltpu.VMEM((tokens, width), bf16),
            slots, pltpu.VMEM((fs // 2, tokens, block_width), jnp.float32), slots, slots, slots,
            dma((2, n)), dma((2, n)), dma((2, 2, n)), dma((2, 2, n)), dma((fs, n)),
            dma((fs, n)), dma((fs, n)), dma((fs, n)), dma((2, DOWN_CUTS)), dma((2, DOWN_CUTS)), dma, dma,
            dma((3,)), dma((2,)), dma, dma,
            dma((fs // 2, HALVES)), dma((fs // 2, HALVES)), dma((fs // 2, HALVES)), dma((fs // 2, HALVES)),
        ],
        compiler_params=pltpu.CompilerParams(
            collective_id=0, has_side_effects=True, vmem_limit_bytes=LAYER_VMEM),
    )(tok, gain, gate, up, down)


def deliver_kernel(pairs, *refs):
    srcs, dsts, sems = refs[:pairs[-1][0] + 1], refs[pairs[-1][0] + 1:-1], refs[-1]
    copies = []
    for (i, view, cuts), dst in zip(pairs, dsts):
        src = srcs[i] if view is None else srcs[i].at[view]
        depth = dst.shape[0] // cuts
        copies += [(src.at[pl.ds(k * depth, depth)], dst.at[pl.ds(k * depth, depth)]) for k in range(cuts)]
    copies = [pltpu.make_async_copy(src, dst, sems.at[i]) for i, (src, dst) in enumerate(copies)]
    for copy in copies:
        copy.start()
    for copy in copies:
        copy.wait()


def deliver(srcs, pairs):
    def shape(i, view):
        return srcs[i].shape if view is None else srcs[i].shape[1:]

    return pl.pallas_call(
        functools.partial(deliver_kernel, pairs),
        out_shape=tuple(pltpu.HBM(shape(i, view), srcs[i].dtype) for i, view, _ in pairs),
        in_specs=[pl.BlockSpec(memory_space=pltpu.VMEM)] * len(srcs),
        out_specs=(pl.BlockSpec(memory_space=pltpu.HBM),) * len(pairs),
        scratch_shapes=[pltpu.SemaphoreType.DMA((sum(cuts for _, _, cuts in pairs),))],
        compiler_params=pltpu.CompilerParams(vmem_limit_bytes=2 ** 20),
    )(*srcs)


def by_kernels(prompt_tokens, norm_gain, gate_trained, up_trained, down_trained):
    fs, tp = lax.axis_size("fs"), lax.axis_size("tp")
    both, down, mixed, _ = layer(
        prompt_tokens, norm_gain[None, :], gate_trained, up_trained, down_trained, fs, tp)
    gate_serving, up_serving = deliver((both,), ((0, 0, 8), (0, 1, 8)))
    down_serving, mixed = deliver((down, mixed), ((0, None, 8), (1, None, 1)))
    return gate_serving, up_serving, down_serving, mixed


def gather_by_collectives(gate_cast, up_cast, down_cast):
    fs_count = lax.axis_size("fs")
    down_serving = lax.all_gather(down_cast, "tp", axis=1, tiled=True)

    def serve(cast):
        part = lax.all_to_all(cast, "tp", split_axis=0, concat_axis=1, tiled=True)
        mid = lax.all_to_all(part, "fs", split_axis=1, concat_axis=0, tiled=True)
        share, width = mid.shape[0] // fs_count, mid.shape[1]
        blocks = lax.all_gather(mid.reshape(fs_count, share, width), "tp", axis=1, tiled=True)
        return blocks.reshape(-1, width)

    return serve(gate_cast), serve(up_cast), down_serving


def on_device(prompt_tokens, norm_gain, gate_trained, up_trained, down_trained):
    fs, tp = lax.axis_size("fs"), lax.axis_size("tp")
    routed = fs == 2 * tp and tp == 4
    if routed:
        return by_kernels(prompt_tokens, norm_gain, gate_trained, up_trained, down_trained)
    gate_cast = (gate_trained * norm_gain[:, None]).astype(jnp.bfloat16)
    up_cast = (up_trained * norm_gain[:, None]).astype(jnp.bfloat16)
    down_cast = down_trained.astype(jnp.bfloat16)
    gate_serving, up_serving, down_serving = gather_by_collectives(gate_cast, up_cast, down_cast)
    tokens = prompt_tokens.astype(jnp.float32)
    scale = lax.rsqrt(jnp.mean(tokens * tokens, axis=-1, keepdims=True) + 1e-06)
    normed = (tokens * scale).astype(jnp.bfloat16)
    contract = (((0,), (1,)), ((), ()))
    gate_cols = lax.dot_general(gate_serving, normed, contract, preferred_element_type=jnp.float32)
    up_cols = lax.dot_general(up_serving, normed, contract, preferred_element_type=jnp.float32)
    hidden_cols = (jax.nn.silu(gate_cols) * up_cols).astype(jnp.bfloat16)
    summed = lax.psum_scatter(
        lax.dot_general(
            down_serving, hidden_cols, (((0,), (0,)), ((), ())), preferred_element_type=jnp.float32
        ),
        "fs",
        scatter_dimension=0,
        tiled=True,
    )
    mixed = summed.T.astype(jnp.bfloat16)
    return (gate_serving, up_serving, down_serving, mixed)


def solution(mesh):
    return jax.shard_map(
        on_device,
        mesh=mesh,
        in_specs=(P("tp", None), P("fs"), P("fs", "tp"), P("fs", "tp"), P("fs", "tp")),
        out_specs=(P(None, "fs"), P(None, "fs"), P("fs", None), P("tp", "fs")),
        check_vma=False,
    )
```
